32 devices in a mesh: sp: 16 (over z, y, core), tp: 2 (over x).
Axes of the slice: x: 2, y: 2, z: 4, core: 2. Of those that a mesh axis runs over, the one named last changes fastest.
Arguments:
- queries: bfloat16 [16384, 1024], P('sp', 'tp'), may hold values from -8 to 8
- keyvals: bfloat16 [16384, 8, 128], P('sp', 'tp'), may hold values from -8 to 8
- head_sink_logit: float32 [16], P('tp'), may hold values from 2 to 7
- doc_ids: int32 [16384], P('sp'), may hold values from 0 to 7, never falling along the last dimension, each value on 1 to 4096 neighbouring positions
- stream_in: bfloat16 [16384, 2048], P(('sp', 'tp')), may hold values from -6 to 6
- out_weight: bfloat16 [1024, 2048], replicated, may hold values from -1.5 to 1.5
- first_gain: float32 [2048], replicated, may hold values from 0.1 to 1.9
- up_weight: bfloat16 [2048, 8192], P('sp', 'tp'), may hold values from -0.125 to 0.125
- down_weight: bfloat16 [8192, 2048], P('tp', 'sp'), may hold values from -0.0625 to 0.0625
- second_gain: float32 [2048], replicated, may hold values from 0.1 to 1.9
Outputs:
- layer_out: bfloat16 [16384, 2048], P(('sp', 'tp'))
The draws below stay inside these ranges and needn't reach their ends.
Inputs may be any that keep to these rules, and one draw needn't show every extreme that they name: `doc_ids`: document numbers never fall along the sequence.
All inputs are finite; a program needn't handle non-finite values.
Results may differ from the reference program's by a relative error of at most 0.013.
Values may be sent and summed in bfloat16 or wider, within the bound.
A program may use at most 128 MiB of HBM per device.

```python
import math
import jax
import jax.numpy as jnp
import numpy as np
from jax import lax

D = 2048
FF = 8192
QUERY_HEADS = 16
KEY_VALUE_HEADS = 8
HEAD_SIZE = 64
WINDOW_REACH = 128
PACKED_TOKENS = 16384
N_SP = 16
N_TP = 2


def draw_queries(key, part):
    self_key = jax.random.fold_in(key, 3)
    value_rows = jnp.clip(jax.random.normal(self_key, (PACKED_TOKENS, QUERY_HEADS, HEAD_SIZE), jnp.float32), -6.0, 6.0)
    return value_rows.reshape(PACKED_TOKENS, QUERY_HEADS * HEAD_SIZE).astype(jnp.bfloat16)


def draw_keyvals(key, part):
    self_key = jax.random.fold_in(key, 5)
    value_rows = jnp.clip(jax.random.normal(self_key, (PACKED_TOKENS, KEY_VALUE_HEADS, 2 * HEAD_SIZE), jnp.float32), -6.0, 6.0)
    return value_rows.astype(jnp.bfloat16)


def levels(stream_key, shape, cuts, smallest, high):
    def one(position, shards_of):
        steps = jax.random.uniform(jax.random.fold_in(jax.random.fold_in(stream_key, 6), position), (shards_of,), jnp.float32, smallest / len(cuts), high / len(cuts))
        return jnp.repeat(jnp.exp(steps), shape[position] // shards_of).reshape((-1,) + (1,) * (len(shape) - position - 1))

    level = one(*cuts[0])
    for cut in cuts[1:]:
        level = level * one(*cut)
    return level


def profile(number_of, total, most, slope):
    weights = [(1 << 20) // math.isqrt(grade ** slope) + 1 for grade in range(2, number_of + 1)]
    spare, given = total - most - (number_of - 1), [1] * (number_of - 1)
    while spare > 0:
        movable = [i for i in range(number_of - 1) if given[i] < most]
        pool, remaining = sum([weights[i] for i in movable]), spare
        for i in movable:
            extra = min(most - given[i], max(1, remaining * weights[i] // pool), spare)
            given[i] = given[i] + extra
            spare = spare - extra
    return np.array([most] + given)


def uneven(rng, count, total, most, skew):
    if count == 2:
        one = jax.random.randint(rng, (), max(1, total - most), min(most, total - 1) + 1)
        return jnp.stack([one, total - one])
    lengths = jnp.asarray(profile(count, total, most, skew), jnp.int32)
    couples = (count - 1) // 2
    source_of, sink = lengths[1:1 + 2 * couples:2], lengths[2:2 + 2 * couples:2]
    margin = jnp.minimum(source_of - 1, most - sink)
    passed = jax.random.randint(jax.random.fold_in(rng, 1), (couples,), 0, 1 << 20) % (margin + 1)
    lengths = lengths.at[1:1 + 2 * couples:2].set(source_of - passed).at[2:2 + 2 * couples:2].set(sink + passed)
    return lengths[jax.random.permutation(jax.random.fold_in(rng, 2), count)]


def noise(stream_key, shape, scale, most, shards=(), kind=jnp.bfloat16):
    array = jax.random.normal(stream_key, shape, jnp.float32) * scale
    if len(shards) > 0:
        array = levels(stream_key, shape, shards, -0.22, 0.18) * array
    return jnp.clip(array, min=-most, max=most).astype(kind)


def setup_inputs(seed: int = 0) -> dict:
    seeds = jax.random.split(jax.random.key(seed), 11)
    queries = draw_queries(jax.random.fold_in(seeds[10], 71), 0)
    keyvals = draw_keyvals(jax.random.fold_in(seeds[10], 71), 0)
    head_sink_logit = jnp.clip(2.0 + 5.0 * jax.random.uniform(seeds[2], (QUERY_HEADS,), jnp.float32) ** levels(seeds[2], (QUERY_HEADS,), ((0, 2),), -0.2, 0.2), 2.0, 7.0)
    doc_ids = jnp.searchsorted(jnp.cumsum(uneven(seeds[3], N_SP // 2, PACKED_TOKENS, PACKED_TOKENS // 4, 1)), jnp.arange(PACKED_TOKENS), side="right").astype(jnp.int32)
    stream_in = noise(seeds[4], (PACKED_TOKENS, D), 1.0, 6.0, ((0, 32),))
    out_weight = noise(seeds[5], (QUERY_HEADS * HEAD_SIZE, D), (QUERY_HEADS * HEAD_SIZE // 64) ** -0.5, 1.5)
    first_gain = jnp.clip(1.0 + 0.18 * jax.random.normal(seeds[6], (D,), jnp.float32), 0.1, 1.9)
    up_weight = noise(seeds[7], (D, FF), D ** -0.5, 0.125, ((0, 16), (1, 2)))
    down_weight = noise(seeds[8], (FF, D), FF ** -0.5, 0.0625, ((0, 2), (1, 16)))
    second_gain = jnp.clip(1.0 + 0.18 * jax.random.normal(seeds[9], (D,), jnp.float32), 0.1, 1.9)
    return dict(queries=queries, keyvals=keyvals, head_sink_logit=head_sink_logit, doc_ids=doc_ids, stream_in=stream_in, out_weight=out_weight, first_gain=first_gain, up_weight=up_weight, down_weight=down_weight, second_gain=second_gain)


NEG_LARGE = -1e+30
NORM_EPS = 1e-05

def layer_norm(stream, gain_row):
    centre = lax.optimization_barrier(jnp.mean(stream, axis=-1, keepdims=True))
    shifted = stream - centre
    spread = lax.optimization_barrier(jnp.mean(shifted * shifted, axis=-1, keepdims=True))
    return shifted * lax.rsqrt(spread + NORM_EPS) * gain_row

def window_attention(queries, keyvals, head_sink_logit, doc_ids):
    block_list = PACKED_TOKENS // WINDOW_REACH
    heads_per_group = QUERY_HEADS // KEY_VALUE_HEADS
    score_scale = HEAD_SIZE ** (-0.5)
    query_block_list = queries.astype(jnp.float32).reshape(block_list, WINDOW_REACH, KEY_VALUE_HEADS, heads_per_group, HEAD_SIZE).transpose(2, 0, 1, 3, 4)
    padding_width = jnp.zeros((WINDOW_REACH, KEY_VALUE_HEADS, 2 * HEAD_SIZE), jnp.float32)
    padded_rows = jnp.concatenate([padding_width, keyvals.astype(jnp.float32), padding_width], axis=0).reshape(block_list + 2, WINDOW_REACH, KEY_VALUE_HEADS, 2 * HEAD_SIZE)
    banded = jnp.concatenate([padded_rows[:-2], padded_rows[1:-1], padded_rows[2:]], axis=1).transpose(2, 0, 1, 3)
    doc_pad = jnp.zeros((WINDOW_REACH,), jnp.int32)
    doc_ext = jnp.concatenate([doc_pad, doc_ids, doc_pad]).reshape(block_list + 2, WINDOW_REACH)
    doc_band = jnp.concatenate([doc_ext[:-2], doc_ext[1:-1], doc_ext[2:]], axis=1)
    query_pos = jnp.arange(PACKED_TOKENS, dtype=jnp.int32).reshape(block_list, WINDOW_REACH, 1)
    key_pos = (jnp.arange(block_list, dtype=jnp.int32)[:, None] * WINDOW_REACH + jnp.arange(3 * WINDOW_REACH, dtype=jnp.int32)[None, :] - WINDOW_REACH)[:, None, :]
    allowed = (jnp.abs(query_pos - key_pos) <= WINDOW_REACH) & (key_pos >= 0) & (key_pos < PACKED_TOKENS) & (doc_ids.reshape(block_list, WINDOW_REACH, 1) == doc_band[:, None, :])
    sink_logit_table = head_sink_logit.reshape(KEY_VALUE_HEADS, heads_per_group)

    def one_head(operands):
        query_head, band_head, sink_head = operands
        scores = jnp.einsum('nqgd,nkd->ngqk', query_head, band_head[..., :HEAD_SIZE]) * score_scale
        scores = jnp.where(allowed[:, None], scores, NEG_LARGE)
        sink_col = sink_head[None, :, None, None]
        highest = jnp.maximum(lax.optimization_barrier(jnp.max(scores, axis=-1, keepdims=True)), sink_col)
        powers = jnp.exp(scores - highest)
        denominator = lax.optimization_barrier(jnp.sum(powers, axis=-1, keepdims=True)) + jnp.exp(sink_col - highest)
        weights = lax.optimization_barrier((powers / denominator).astype(jnp.bfloat16)).astype(jnp.float32)
        mixed_out = jnp.einsum('ngqk,nkd->nqgd', weights, band_head[..., HEAD_SIZE:])
        return mixed_out.astype(jnp.bfloat16)
    heads_out = lax.map(one_head, (query_block_list, banded, sink_logit_table))
    return heads_out.transpose(1, 2, 0, 3, 4).reshape(PACKED_TOKENS, QUERY_HEADS * HEAD_SIZE)

def reference(queries, keyvals, head_sink_logit, doc_ids, stream_in, out_weight, first_gain, up_weight, down_weight, second_gain):
    attended = window_attention(queries, keyvals, head_sink_logit, doc_ids)
    projected = jnp.dot(attended, out_weight, preferred_element_type=jnp.float32)
    first_stream = layer_norm(stream_in.astype(jnp.float32) + projected, first_gain).astype(jnp.bfloat16)
    ff_share = FF // N_TP
    up_groups = up_weight.reshape(D, N_TP, ff_share).transpose(1, 0, 2)
    down_groups = down_weight.reshape(N_TP, ff_share, D)

    def add_group(running, weight_pair):
        up_part, down_part = weight_pair
        hidden = jnp.dot(first_stream, up_part, preferred_element_type=jnp.float32)
        active = jnp.square(jnp.maximum(hidden, 0.0)).astype(jnp.bfloat16)
        partial_value = jnp.dot(active, down_part, preferred_element_type=jnp.float32)
        rounded = lax.optimization_barrier(partial_value.astype(jnp.bfloat16)).astype(jnp.float32)
        return (running + rounded, None)
    mixed_out, unused_out = lax.scan(add_group, jnp.zeros((PACKED_TOKENS, D), jnp.float32), (up_groups, down_groups))
    return layer_norm(first_stream.astype(jnp.float32) + mixed_out, second_gain).astype(jnp.bfloat16)
```

```python
import jax
import jax.numpy as jnp
from jax import lax
from jax.experimental import pallas as pl
from jax.sharding import PartitionSpec as P

HEAD_SIZE = 64
WINDOW_REACH = 128


NEG_LARGE = -1e30
NORM_EPS = 1e-05


def padded(block, sides, width):
    for axis, dim in sides:
        count = lax.axis_size(axis)
        forward = [(i, i + 1) for i in range(count - 1)]
        backward = [(target, source) for source, target in forward]
        low = lax.ppermute(
            lax.slice_in_dim(block, block.shape[dim] - width, None, axis=dim), axis, forward
        )
        high = lax.ppermute(lax.slice_in_dim(block, 0, width, axis=dim), axis, backward)
        block = jnp.concatenate([low, block, high], axis=dim)
    return block


def layer_norm(stream, gain_row):
    centre = jnp.mean(stream, axis=-1, keepdims=True)
    shifted = stream - centre
    spread = jnp.mean(shifted * shifted, axis=-1, keepdims=True)
    return shifted * lax.rsqrt(spread + NORM_EPS) * gain_row


def attend(queries, keyvals, head_sink_logit, doc_ids):
    tok_rows = queries.shape[0]
    kv_heads = keyvals.shape[1]
    heads_per_group = queries.shape[1] // (HEAD_SIZE * kv_heads)
    block_list = tok_rows // WINDOW_REACH
    score_scale = HEAD_SIZE ** (-0.5)
    doc_marks = doc_ids.astype(jnp.bfloat16)
    rim_keys, rim_docs = (
        padded(keyvals, (("sp", 0),), WINDOW_REACH),
        padded(doc_marks, (("sp", 0),), WINDOW_REACH),
    )
    padded_rows = rim_keys.reshape(block_list + 2, WINDOW_REACH, kv_heads, 2 * HEAD_SIZE)
    banded = jnp.concatenate([padded_rows[:-2], padded_rows[1:-1], padded_rows[2:]], axis=1)
    doc_ext = rim_docs.reshape(block_list + 2, WINDOW_REACH)
    doc_band = jnp.concatenate([doc_ext[:-2], doc_ext[1:-1], doc_ext[2:]], axis=1)
    offset = lax.axis_index("sp") * tok_rows
    total_rows = tok_rows * lax.axis_size("sp")
    query_pos = offset + jnp.arange(tok_rows, dtype=jnp.int32).reshape(block_list, WINDOW_REACH, 1)
    key_pos = (
        offset
        + (
            jnp.arange(block_list, dtype=jnp.int32)[:, None] * WINDOW_REACH
            + jnp.arange(3 * WINDOW_REACH, dtype=jnp.int32)[None, :]
            - WINDOW_REACH
        )[:, None, :]
    )
    allowed = (
        (jnp.abs(query_pos - key_pos) <= WINDOW_REACH)
        & (key_pos >= 0)
        & (key_pos < total_rows)
        & (doc_marks.reshape(block_list, WINDOW_REACH, 1) == doc_band[:, None, :])
    )
    query_block_list = queries.reshape(
        block_list, WINDOW_REACH, kv_heads, heads_per_group, HEAD_SIZE
    )
    scores = (
        jnp.einsum(
            "nqhgd,nkhd->nhgqk",
            query_block_list,
            banded[..., :HEAD_SIZE],
            preferred_element_type=jnp.float32,
        )
        * score_scale
    )
    scores = jnp.where(allowed[:, None, None], scores, NEG_LARGE)
    sink_col = head_sink_logit.reshape(kv_heads, heads_per_group)[None, :, :, None, None]
    highest = jnp.maximum(jnp.max(scores, axis=-1, keepdims=True), sink_col)
    powers = jnp.exp(scores - highest)
    denominator = jnp.sum(powers, axis=-1, keepdims=True) + jnp.exp(sink_col - highest)
    weights = (powers / denominator).astype(jnp.bfloat16)
    mixed_out = jnp.einsum(
        "nhgqk,nkhd->nqhgd", weights, banded[..., HEAD_SIZE:], preferred_element_type=jnp.float32
    )
    return mixed_out.astype(jnp.bfloat16).reshape(tok_rows, kv_heads * heads_per_group * HEAD_SIZE)


def cyclic(block, axis, shift):
    count = lax.axis_size(axis)
    return lax.ppermute(block, axis, [(i, (i + shift) % count) for i in range(count)])


def gather_columns(block, axis):
    count = lax.axis_size(axis)
    line_count = count // 4
    me = lax.axis_index(axis)
    line, side = me // 4, me % 2
    rows, width = block.shape

    def along(shift):
        return [(i, (i + 4 * shift) % count) for i in range(count)]

    across = [(i, i ^ 2) for i in range(count)]
    beside = [(i, i ^ 1) for i in range(count)]
    this_row = [block] + [lax.ppermute(block, axis, along(shift)) for shift in range(1, line_count)]
    other_row = [lax.ppermute(block, axis, across)]
    other_row += [lax.ppermute(piece, axis, across) for piece in this_row[1:]]

    row = (me // 2) % 2
    whole = jnp.zeros((rows, count * width), block.dtype)
    for pieces, from_row in ((this_row, row), (other_row, 1 - row)):
        for shift, piece in enumerate(pieces):
            source = lax.rem(line - shift + line_count, line_count)
            partner = lax.ppermute(piece, axis, beside)
            first = 4 * source + 2 * from_row
            whole = lax.dynamic_update_slice(whole, piece, (0, (first + side) * width))
            whole = lax.dynamic_update_slice(whole, partner, (0, (first + 1 - side) * width))
    return whole


def per_device(
    queries,
    keyvals,
    head_sink_logit,
    doc_ids,
    stream_in,
    out_weight,
    first_gain,
    up_weight,
    down_weight,
    second_gain,
):
    up_whole = lax.all_gather(up_weight, "sp", axis=0, tiled=True)
    cut = down_weight.shape[0] // 2
    down_low = lax.all_gather(down_weight[:cut], "sp", axis=1, tiled=True)
    down_high = gather_columns(down_weight[cut:], "sp")
    attended = attend(queries, keyvals, head_sink_logit, doc_ids)
    tp_count = lax.axis_size("tp")
    own_rows = attended.shape[0] // tp_count
    by_peer = attended.reshape(tp_count, own_rows, attended.shape[1])
    projected = jnp.dot(
        lax.all_to_all(by_peer, "tp", split_axis=0, concat_axis=2, tiled=True)[0],
        out_weight,
        preferred_element_type=jnp.float32,
    )
    first_stream = layer_norm(stream_in.astype(jnp.float32) + projected, first_gain).astype(
        jnp.bfloat16
    )

    def activate(rows):
        hidden = jnp.dot(rows, up_whole, preferred_element_type=jnp.float32)
        return lax.optimization_barrier(jnp.square(jnp.maximum(hidden, 0.0)).astype(jnp.bfloat16))

    def contract(active):
        early = lax.optimization_barrier(
            jnp.dot(active[:, cut:], down_high, preferred_element_type=jnp.float32)
        )
        late = jnp.dot(active[:, :cut], down_low, preferred_element_type=jnp.float32)
        return lax.optimization_barrier((early + late).astype(jnp.bfloat16))

    visiting = [cyclic(first_stream, "tp", shift) for shift in range(1, tp_count)]
    own_active = activate(first_stream)
    visiting_active = [activate(rows) for rows in visiting]
    visiting_parts = [contract(active) for active in visiting_active]
    returned = [cyclic(part, "tp", -shift) for shift, part in enumerate(visiting_parts, 1)]
    own_part = contract(own_active)
    return closing_norm(first_stream, second_gain, [own_part] + returned)


def closing_kernel(stream_ref, gain_ref, *refs):
    mixed = refs[0][...].astype(jnp.float32)
    for partial_ref in refs[1:-1]:
        mixed = mixed + partial_ref[...].astype(jnp.float32)
    refs[-1][...] = layer_norm(
        stream_ref[...].astype(jnp.float32) + mixed, gain_ref[...]
    ).astype(refs[-1].dtype)


def closing_norm(stream, gain, partials):
    rows, width = stream.shape
    tile = min(128, rows)
    row_spec = pl.BlockSpec((tile, width), lambda i: (i, 0))
    return pl.pallas_call(
        closing_kernel,
        grid=(rows // tile,),
        out_shape=jax.ShapeDtypeStruct(stream.shape, stream.dtype),
        in_specs=[row_spec, pl.BlockSpec((1, width), lambda i: (0, 0))]
        + [row_spec] * len(partials),
        out_specs=row_spec,
        name="closing_norm",
    )(stream, gain.reshape(1, width), *partials)


def solution(mesh):
    return jax.shard_map(
        per_device,
        mesh=mesh,
        in_specs=(
            P("sp", "tp"),
            P("sp", "tp", None),
            P("tp"),
            P("sp"),
            P(("sp", "tp"), None),
            P(),
            P(),
            P("sp", "tp"),
            P("tp", "sp"),
            P(),
        ),
        out_specs=P(("sp", "tp"), None),
        check_vma=False,
    )
```
